32 devices in a mesh: ep: 8 (over z, y), tp: 4 (over x, core).
Axes of the slice: x: 2, y: 2, z: 4, core: 2. Of those that a mesh axis runs over, the one named last changes fastest.
Arguments:
- tokens: bfloat16 [2048, 1024], P('ep'), may hold values from -6 to 6
- cotangent: bfloat16 [2048, 1024], P('ep'), may hold values from -1.5 to 1.5
- routing: int32 [2048, 2], P('ep'), may hold values from 0 to 15, all different within a row; in each aligned block of 256 rows (0 to 255, 256 to 511, ...) at most 96 rows name the same one
- gate_weights: float32 [2048, 2], P('ep'), may hold values from 0.1 to 0.9
- gate_proj: bfloat16 [16, 1024, 512], P('ep', None, 'tp'), may hold values from -0.1875 to 0.1875
- up_proj: bfloat16 [16, 1024, 512], P('ep', None, 'tp'), may hold values from -0.1875 to 0.1875
- down_proj: bfloat16 [16, 512, 1024], P('ep', 'tp'), may hold values from -0.25 to 0.25
Outputs:
- tokens_grad: bfloat16 [2048, 1024], P('ep')
- gates_grad: float32 [2048, 2], P('ep')
- gate_proj_grad: float32 [16, 1024, 512], P('ep', None, 'tp')
- up_proj_grad: float32 [16, 1024, 512], P('ep', None, 'tp')
- down_proj_grad: float32 [16, 512, 1024], P('ep', 'tp')
The draws below stay inside these ranges and needn't reach their ends.
Inputs may be any that keep to these rules, and one draw needn't show every extreme that they name: `routing`: each row names 2 different experts; every expert is named by some row; within each aligned block of 256 rows (the tokens of one index of ep) no expert is named by more than 96 rows, a bound that some block reaches.
All inputs are finite; a program needn't handle non-finite values.
Results may differ from the reference program's by a relative error of at most 0.0015.
Values may be sent and summed in bfloat16 or wider, within the bound.
A program may use at most 128 MiB of HBM per device.

```python
import math
import jax
import jax.numpy as jnp
import numpy as np
from jax import lax

D = 1024
FF = 512
TOP = 2
TOK_DEV = 256
EXPERTS = 16
TOKENS = 2048
CAP = 96
N_EP = 8


def steps_of(own_key, shape, split, least, high):
    factor_of = 1.0
    for axis_at, parts in split:
        heights = jax.random.uniform(jax.random.fold_in(jax.random.fold_in(own_key, 6), axis_at), (parts,), jnp.float32, least / len(split), high / len(split))
        factor_of = factor_of * jnp.repeat(jnp.exp(heights), shape[axis_at] // parts).reshape((-1,) + (1,) * (len(shape) - 1 - axis_at))
    return factor_of


def shared_out(own_key, own, number, rows, number_of, top, reach, slope):
    sequence = jax.random.permutation(own_key, number_of)
    heavy_load, common = shares(number_of, rows * top, reach, slope, True), shares(number_of, rows * top, reach, slope, False)
    places = jnp.arange(number_of)

    def named(tallies, rotation):
        used = int((tallies > 0).sum())
        fixed = max(1, used // 4)
        moved = fixed + (places - fixed + rotation * (used - fixed)) % max(1, number_of - fixed)
        return jnp.zeros((number_of,), jnp.int32).at[sequence[jnp.where(places < fixed, places, moved)]].set(jnp.asarray(tallies, jnp.int32))

    tallies = jnp.where(number % 4 == 0, named(heavy_load, number // 4), named(common, number - number // 4 - 1))
    mixed = jax.random.permutation(jax.random.fold_in(own, 3), number_of)
    giver, sink = mixed[0:number_of // 2 * 2:2], mixed[1:number_of // 2 * 2:2]
    slack = jnp.minimum(tallies[giver] - 1, reach - tallies[sink]) // 2
    slack = jnp.where((giver == sequence[0]) | (sink == sequence[0]) | (tallies[sink] == 0), 0, jnp.maximum(slack, 0))
    moved = jax.random.randint(jax.random.fold_in(own, 4), (number_of // 2,), 0, 1 << 20) % (slack + 1)
    tallies = tallies.at[giver].add(-moved).at[sink].add(moved)
    labels = jnp.searchsorted(jnp.cumsum(tallies), jnp.arange(rows * top), side="right").astype(jnp.int32)
    listing = labels.reshape(top, rows).T
    listing = listing[jax.random.permutation(jax.random.fold_in(own, 1), rows)]
    rotation = jax.random.randint(jax.random.fold_in(own, 2), (rows, 1), 0, top)
    return jnp.take_along_axis(listing, (jnp.arange(top)[None, :] + rotation) % top, axis=1)


def shares(amount, total, limit, skew, full):
    portions = [(1 << 20) // math.isqrt(rank ** skew) + 1 for rank in range(1, amount + 1)]
    largest = limit if full else min(limit, max(-(-total // amount), total * portions[0] // sum(portions)))
    least = 1 if total - largest >= amount - 1 else 0
    counts, surplus = [largest] + [least] * (amount - 1), total - largest - least * (amount - 1)
    while surplus > 0:
        free = [i for i in range(1, amount) if counts[i] < largest] or [i for i in range(1, amount) if counts[i] < limit]
        pool, left = sum([portions[i] for i in free]), surplus
        for i in free:
            more = min(limit - counts[i], max(1, left * portions[i] // pool), surplus)
            counts[i] = counts[i] + more
            surplus = surplus - more
    return np.array(counts)


def gaussian(own_key, dims, scale, reach, shards=(), kind=jnp.bfloat16):
    loudness = steps_of(own_key, dims, shards, -0.22, 0.18) if shards else 1.0
    entries = jax.random.normal(own_key, dims, jnp.float32) * scale * loudness
    return jnp.minimum(jnp.maximum(entries, -reach), reach).astype(kind)


def setup_inputs(seed: int = 0) -> dict:
    streams_of = jax.random.split(jax.random.key(seed), 8)
    tokens = gaussian(streams_of[0], (TOKENS, D), 1.0, 6.0, ((0, 8),))
    cotangent = gaussian(streams_of[1], (TOKENS, D), 0.25, 1.5, ((0, 8),))
    routing_keys = jax.random.split(jax.random.fold_in(streams_of[2], 1), TOKENS // TOK_DEV)
    routing_turns = jax.random.permutation(jax.random.fold_in(streams_of[2], 3), TOKENS // TOK_DEV)
    routing = jax.vmap(lambda own, number: shared_out(jax.random.fold_in(streams_of[2], 2), own, number, TOK_DEV, EXPERTS, TOP, CAP, 2))(routing_keys, routing_turns).reshape((TOKENS, TOP))
    gate_weights = jnp.clip(0.1 + 0.79999997 * jax.random.uniform(streams_of[3], (TOKENS, TOP), jnp.float32) ** steps_of(streams_of[3], (TOKENS, TOP), ((0, 8),), -0.2, 0.2), 0.1, 0.9)
    gate_proj = gaussian(streams_of[4], (EXPERTS, D, FF), D ** -0.5, 0.1875, ((0, 8), (2, 4)))
    up_proj = gaussian(streams_of[5], (EXPERTS, D, FF), D ** -0.5, 0.1875, ((0, 8), (2, 4)))
    down_proj = gaussian(streams_of[6], (EXPERTS, FF, D), FF ** -0.5, 0.25, ((0, 8), (1, 4)))
    return dict(tokens=tokens, cotangent=cotangent, routing=routing, gate_weights=gate_weights, gate_proj=gate_proj, up_proj=up_proj, down_proj=down_proj)


def expert_pass(expert_rows, scaled, gate_matrix, up_matrix, down_matrix):
    gate_pre = jnp.dot(expert_rows, gate_matrix, preferred_element_type=jnp.float32).astype(jnp.bfloat16)
    up_pre = jnp.dot(expert_rows, up_matrix, preferred_element_type=jnp.float32).astype(jnp.bfloat16)
    gate_pre, up_pre = lax.optimization_barrier((gate_pre, up_pre))
    hidden_grad = jnp.dot(scaled, down_matrix.T, preferred_element_type=jnp.float32)
    gate_wide = gate_pre.astype(jnp.float32)
    up_wide = up_pre.astype(jnp.float32)
    sigmoid_gate = jax.nn.sigmoid(gate_wide)
    activated = gate_wide * sigmoid_gate
    hidden = activated * up_wide
    product = jnp.sum(hidden_grad * hidden, axis=-1)
    gate_pre_grad = (hidden_grad * up_wide * sigmoid_gate * (1.0 + gate_wide * (1.0 - sigmoid_gate))).astype(jnp.bfloat16)
    up_pre_grad = (hidden_grad * activated).astype(jnp.bfloat16)
    input_grad = jnp.dot(gate_pre_grad, gate_matrix.T, preferred_element_type=jnp.float32)
    input_grad = input_grad + jnp.dot(up_pre_grad, up_matrix.T, preferred_element_type=jnp.float32)
    down_grad = jnp.dot(hidden.astype(jnp.bfloat16).T, scaled, preferred_element_type=jnp.float32)
    gate_grad = jnp.dot(expert_rows.T, gate_pre_grad, preferred_element_type=jnp.float32)
    up_grad = jnp.dot(expert_rows.T, up_pre_grad, preferred_element_type=jnp.float32)
    return input_grad, product, gate_grad, up_grad, down_grad


def reference(tokens, cotangent, routing, gate_weights, gate_proj, up_proj, down_proj):
    pair_count = TOKENS * TOP
    row_limit = N_EP * CAP
    pair_expert = routing.reshape(pair_count)
    pair_weight = gate_weights.reshape(pair_count)

    def one_expert(expert_index):
        chosen = jnp.nonzero(pair_expert == expert_index, size=row_limit, fill_value=pair_count)[0].astype(jnp.int32)
        is_valid = chosen < pair_count
        safe_index = jnp.where(is_valid, chosen, 0).astype(jnp.int32)
        token_index = (safe_index // TOP).astype(jnp.int32)
        expert_rows = jnp.where(is_valid[:, None], tokens[token_index], jnp.zeros((), tokens.dtype))
        weight = jnp.where(is_valid, pair_weight[safe_index], jnp.zeros((), pair_weight.dtype))
        scaled = (weight[:, None] * cotangent[token_index].astype(jnp.float32)).astype(jnp.bfloat16)
        terms = expert_pass(expert_rows, scaled, gate_proj[expert_index], up_proj[expert_index], down_proj[expert_index])
        return (chosen,) + terms

    chosen, input_grad, product, gate_grad, up_grad, down_grad = lax.map(one_expert, jnp.arange(EXPERTS, dtype=jnp.int32))
    flat_chosen = chosen.reshape(-1)
    pair_grad = jnp.zeros((pair_count + 1, D), jnp.float32).at[flat_chosen].set(input_grad.reshape(-1, D))
    pair_product = jnp.zeros((pair_count + 1,), jnp.float32).at[flat_chosen].set(product.reshape(-1))
    tokens_grad = jnp.sum(pair_grad[:pair_count].reshape(TOKENS, TOP, D), axis=1).astype(jnp.bfloat16)
    gates_grad = (pair_product[:pair_count] / pair_weight).reshape(TOKENS, TOP)
    return tokens_grad, gates_grad, gate_grad, up_grad, down_grad
```

```python
import jax
import jax.numpy as jnp
from jax import lax
from jax.sharding import PartitionSpec as P


def expert_terms(expert_rows, expert_scaled, gate_proj, up_proj, down_proj):
    gate_pre = jnp.einsum(
        "erd,edf->erf", expert_rows, gate_proj, preferred_element_type=jnp.float32
    ).astype(jnp.bfloat16)
    up_pre = jnp.einsum(
        "erd,edf->erf", expert_rows, up_proj, preferred_element_type=jnp.float32
    ).astype(jnp.bfloat16)
    gate_pre, up_pre = lax.optimization_barrier((gate_pre, up_pre))
    hidden_grad = jnp.einsum(
        "erd,efd->erf", expert_scaled, down_proj, preferred_element_type=jnp.float32
    )
    gate_wide = gate_pre.astype(jnp.float32)
    up_wide = up_pre.astype(jnp.float32)
    sigmoid_gate = jax.nn.sigmoid(gate_wide)
    activated = gate_wide * sigmoid_gate
    hidden = activated * up_wide
    product = jnp.sum(hidden_grad * hidden, axis=-1)
    gate_pre_grad = (
        hidden_grad * up_wide * sigmoid_gate * (1.0 + gate_wide * (1.0 - sigmoid_gate))
    ).astype(jnp.bfloat16)
    up_pre_grad = (hidden_grad * activated).astype(jnp.bfloat16)
    input_grad = jnp.einsum(
        "erf,edf->erd", gate_pre_grad, gate_proj, preferred_element_type=jnp.float32
    )
    input_grad = input_grad + jnp.einsum(
        "erf,edf->erd", up_pre_grad, up_proj, preferred_element_type=jnp.float32
    )
    down_grad = jnp.einsum(
        "erf,erd->efd",
        hidden.astype(jnp.bfloat16),
        expert_scaled,
        preferred_element_type=jnp.float32,
    )
    gate_grad = jnp.einsum(
        "erd,erf->edf", expert_rows, gate_pre_grad, preferred_element_type=jnp.float32
    )
    up_grad = jnp.einsum(
        "erd,erf->edf", expert_rows, up_pre_grad, preferred_element_type=jnp.float32
    )
    return (input_grad, product, gate_grad, up_grad, down_grad)


def slot_shards(tokens, cotangent, routing, gate_weights, gate_proj, up_proj, down_proj):
    token_count, model_width = tokens.shape
    top_count = routing.shape[1]
    local_experts = gate_proj.shape[0]
    groups = lax.axis_size("ep")
    members = lax.axis_size("tp")
    experts = local_experts * groups
    capacity = members * (
        (3 * token_count * top_count + experts * members - 1) // (experts * members)
    )
    slot_count = experts * capacity
    pair_count = token_count * top_count
    pair_expert = routing.reshape(pair_count)
    onehot = (pair_expert[:, None] == jnp.arange(experts, dtype=jnp.int32)[None, :]).astype(
        jnp.int32
    )
    position = jnp.sum(jnp.cumsum(onehot, axis=0) * onehot, axis=1) - 1
    pair_slot = pair_expert * capacity + position
    pair_number = jnp.arange(pair_count, dtype=jnp.int32)
    owner_pair = jnp.zeros((slot_count,), jnp.int32).at[pair_slot].set(pair_number)
    filled = jnp.zeros((slot_count,), jnp.int32).at[pair_slot].set(1) > 0
    owner_token = owner_pair // top_count
    slot_weight = jnp.where(filled, gate_weights.reshape(pair_count)[owner_pair], 0.0)
    send_rows = jnp.where(filled[:, None], tokens[owner_token], jnp.zeros((), jnp.bfloat16))
    send_scaled = (slot_weight[:, None] * cotangent[owner_token].astype(jnp.float32)).astype(
        jnp.bfloat16
    )
    layout = (groups, local_experts, capacity, model_width)
    send_rows = send_rows.reshape(layout)
    send_scaled = send_scaled.reshape(layout)
    quarter = capacity // members
    quarter_start = lax.axis_index("tp") * quarter
    part_rows = lax.dynamic_slice_in_dim(send_rows, quarter_start, quarter, 2)
    part_scaled = lax.dynamic_slice_in_dim(send_scaled, quarter_start, quarter, 2)
    landed = (
        lax.all_to_all(part_rows, "ep", split_axis=0, concat_axis=0, tiled=True),
        lax.all_to_all(part_scaled, "ep", split_axis=0, concat_axis=0, tiled=True),
    )
    recv_rows, recv_scaled = (
        lax.all_gather(landed[0], "tp", axis=2, tiled=True),
        lax.all_gather(landed[1], "tp", axis=2, tiled=True),
    )
    expert_rows = recv_rows.transpose(1, 0, 2, 3).reshape(
        local_experts, groups * capacity, model_width
    )
    expert_scaled = recv_scaled.transpose(1, 0, 2, 3).reshape(
        local_experts, groups * capacity, model_width
    )
    input_grad, product, gate_grad, up_grad, down_grad = expert_terms(
        expert_rows, expert_scaled, gate_proj, up_proj, down_proj
    )
    input_grad = input_grad.reshape(local_experts, groups, capacity, model_width).transpose(
        1, 0, 2, 3
    )
    product = product.reshape(local_experts, groups, capacity).transpose(1, 0, 2)
    back_grad, back_product = (
        lax.all_to_all(input_grad, "ep", split_axis=0, concat_axis=0, tiled=True),
        lax.all_to_all(product, "ep", split_axis=0, concat_axis=0, tiled=True),
    )
    local_slot = position
    present = (local_slot >= 0) & (local_slot < capacity)
    back_index = pair_expert * capacity + jnp.clip(local_slot, 0, capacity - 1)
    pair_grad = jnp.where(
        present[:, None], back_grad.reshape(experts * capacity, model_width)[back_index], 0.0
    )
    pair_product = jnp.where(present, back_product.reshape(experts * capacity)[back_index], 0.0)
    token_grad = jnp.sum(pair_grad.reshape(token_count, top_count, model_width), axis=1)
    total_grad, total_product = lax.psum((token_grad, pair_product), "tp")
    tokens_grad = total_grad.astype(jnp.bfloat16)
    gates_grad = (total_product / gate_weights.reshape(pair_count)).reshape(token_count, top_count)
    return (tokens_grad, gates_grad, gate_grad, up_grad, down_grad)


def dense_shards(tokens, cotangent, routing, gate_weights, gate_proj, up_proj, down_proj):
    token_count, model_width = tokens.shape
    local_experts = gate_proj.shape[0]
    groups = lax.axis_size("ep")
    members = lax.axis_size("tp")
    experts = local_experts * groups
    all_axes = ("ep", "tp")
    quarter = token_count // members
    quarter_start = lax.axis_index("tp") * quarter
    both = jnp.concatenate(
        [
            lax.dynamic_slice_in_dim(tokens, quarter_start, quarter, 0),
            lax.dynamic_slice_in_dim(cotangent, quarter_start, quarter, 0),
        ],
        axis=1,
    )
    all_both = lax.all_gather(both, all_axes, axis=0, tiled=True)
    chosen = routing[:, :, None] == jnp.arange(experts, dtype=jnp.int32)[None, None, :]
    weights = jnp.sum(jnp.where(chosen, gate_weights[:, :, None], 0.0), axis=1)
    all_weights = lax.all_gather(weights, "ep", axis=0, tiled=True)
    first_expert = lax.axis_index("ep") * local_experts
    my_weights = lax.dynamic_slice_in_dim(all_weights, first_expert, local_experts, 1)
    all_tokens = all_both[:, :model_width]
    all_cotangent = all_both[:, model_width:].astype(jnp.float32)
    rows = jnp.broadcast_to(all_tokens[None], (local_experts,) + all_tokens.shape)
    scaled = (my_weights.T[:, :, None] * all_cotangent[None]).astype(jnp.bfloat16)
    input_grad, product, gate_grad, up_grad, down_grad = expert_terms(
        rows, scaled, gate_proj, up_proj, down_proj
    )
    partial = jnp.sum(input_grad, axis=0)
    own = jnp.zeros((token_count * groups, experts), jnp.float32)
    own = lax.dynamic_update_slice_in_dim(own, product.T, first_expert, 1)
    part_grad = lax.psum_scatter(partial, all_axes, scatter_dimension=0, tiled=True)
    part_product = lax.psum_scatter(own, all_axes, scatter_dimension=0, tiled=True)
    tokens_grad = lax.all_gather(part_grad.astype(jnp.bfloat16), "tp", axis=0, tiled=True)
    block_product = lax.all_gather(part_product, "tp", axis=0, tiled=True)
    pair_product = jnp.sum(jnp.where(chosen, block_product[:, None, :], 0.0), axis=2)
    gates_grad = pair_product / gate_weights
    return (tokens_grad, gates_grad, gate_grad, up_grad, down_grad)


def shards(tokens, cotangent, routing, gate_weights, gate_proj, up_proj, down_proj):
    token_count = tokens.shape[0]
    experts = gate_proj.shape[0] * lax.axis_size("ep")
    members = lax.axis_size("tp")
    fair = token_count * routing.shape[1] // experts
    dense = token_count <= 8 * fair and token_count % members == 0
    plan = dense_shards if dense else slot_shards
    return plan(tokens, cotangent, routing, gate_weights, gate_proj, up_proj, down_proj)


def solution(mesh):
    in_specs = (
        P("ep", None),
        P("ep", None),
        P("ep", None),
        P("ep", None),
        P("ep", None, "tp"),
        P("ep", None, "tp"),
        P("ep", "tp", None),
    )
    out_specs = (
        P("ep", None),
        P("ep", None),
        P("ep", None, "tp"),
        P("ep", None, "tp"),
        P("ep", "tp", None),
    )
    return jax.shard_map(shards, mesh=mesh, in_specs=in_specs, out_specs=out_specs, check_vma=False)
```

```python
import jax
import jax.numpy as jnp
from jax import lax
from jax.sharding import PartitionSpec as P


def expert_terms(expert_rows, expert_scaled, gate_proj, up_proj, down_proj):
    gate_pre = jnp.einsum(
        "erd,edf->erf", expert_rows, gate_proj, preferred_element_type=jnp.float32
    ).astype(jnp.bfloat16)
    up_pre = jnp.einsum(
        "erd,edf->erf", expert_rows, up_proj, preferred_element_type=jnp.float32
    ).astype(jnp.bfloat16)
    gate_pre, up_pre = lax.optimization_barrier((gate_pre, up_pre))
    hidden_grad = jnp.einsum(
        "erd,efd->erf", expert_scaled, down_proj, preferred_element_type=jnp.float32
    )
    gate_wide = gate_pre.astype(jnp.float32)
    up_wide = up_pre.astype(jnp.float32)
    sigmoid_gate = jax.nn.sigmoid(gate_wide)
    activated = gate_wide * sigmoid_gate
    hidden = activated * up_wide
    product = jnp.sum(hidden_grad * hidden, axis=-1)
    gate_pre_grad = (
        hidden_grad * up_wide * sigmoid_gate * (1.0 + gate_wide * (1.0 - sigmoid_gate))
    ).astype(jnp.bfloat16)
    up_pre_grad = (hidden_grad * activated).astype(jnp.bfloat16)
    input_grad = jnp.einsum(
        "erf,edf->erd", gate_pre_grad, gate_proj, preferred_element_type=jnp.float32
    )
    input_grad = input_grad + jnp.einsum(
        "erf,edf->erd", up_pre_grad, up_proj, preferred_element_type=jnp.float32
    )
    down_grad = jnp.einsum(
        "erf,erd->efd",
        hidden.astype(jnp.bfloat16),
        expert_scaled,
        preferred_element_type=jnp.float32,
    )
    gate_grad = jnp.einsum(
        "erd,erf->edf", expert_rows, gate_pre_grad, preferred_element_type=jnp.float32
    )
    up_grad = jnp.einsum(
        "erd,erf->edf", expert_rows, up_pre_grad, preferred_element_type=jnp.float32
    )
    return (input_grad, product, gate_grad, up_grad, down_grad)


def shards(tokens, cotangent, routing, gate_weights, gate_proj, up_proj, down_proj):
    token_count, model_width = tokens.shape
    top_count = routing.shape[1]
    local_experts = gate_proj.shape[0]
    groups = lax.axis_size("ep")
    members = lax.axis_size("tp")
    experts = local_experts * groups
    capacity = members * (
        (3 * token_count * top_count + experts * members - 1) // (experts * members)
    )
    slot_count = experts * capacity
    pair_count = token_count * top_count
    pair_expert = routing.reshape(pair_count)
    onehot = (pair_expert[:, None] == jnp.arange(experts, dtype=jnp.int32)[None, :]).astype(
        jnp.int32
    )
    position = jnp.sum(jnp.cumsum(onehot, axis=0) * onehot, axis=1) - 1
    pair_slot = pair_expert * capacity + position
    token_slot = pair_slot.reshape(token_count, top_count)
    quarter = capacity // members
    quarter_start = lax.axis_index("tp") * quarter
    slot_ids = (
        jnp.arange(experts, dtype=jnp.int32)[:, None] * capacity
        + quarter_start
        + jnp.arange(quarter, dtype=jnp.int32)[None, :]
    ).reshape(experts * quarter)
    pick = jnp.zeros((experts * quarter, token_count), jnp.bool_)
    pick_weight = jnp.zeros((experts * quarter, token_count), jnp.float32)
    for k in range(top_count):
        match = token_slot[:, k][None, :] == slot_ids[:, None]
        pick = pick | match
        pick_weight = jnp.where(match, gate_weights[:, k][None, :], pick_weight)
    pick = pick.astype(jnp.bfloat16)
    slot_weight = jnp.sum(pick_weight, axis=1)
    layout = (groups, local_experts, quarter, model_width)
    part_rows = jnp.dot(pick, tokens, preferred_element_type=jnp.float32)
    part_rows = part_rows.astype(jnp.bfloat16).reshape(layout)
    part_scaled = jnp.dot(pick, cotangent, preferred_element_type=jnp.float32)
    part_scaled = (slot_weight[:, None] * part_scaled).astype(jnp.bfloat16).reshape(layout)
    landed = (
        lax.all_to_all(part_rows, "ep", split_axis=0, concat_axis=0, tiled=True),
        lax.all_to_all(part_scaled, "ep", split_axis=0, concat_axis=0, tiled=True),
    )
    recv_rows, recv_scaled = (
        lax.all_gather(landed[0], "tp", axis=2, tiled=True),
        lax.all_gather(landed[1], "tp", axis=2, tiled=True),
    )
    expert_rows = recv_rows.transpose(1, 0, 2, 3).reshape(
        local_experts, groups * capacity, model_width
    )
    expert_scaled = recv_scaled.transpose(1, 0, 2, 3).reshape(
        local_experts, groups * capacity, model_width
    )
    input_grad, product, gate_grad, up_grad, down_grad = expert_terms(
        expert_rows, expert_scaled, gate_proj, up_proj, down_proj
    )
    peak = jnp.maximum(jnp.max(jnp.abs(input_grad), axis=-1), 1e-30)
    narrow = (input_grad * (1.0 / peak)[:, :, None]).astype(jnp.float16)
    narrow = narrow.reshape(local_experts, groups, capacity, model_width).transpose(1, 0, 2, 3)
    extras = jnp.stack([product, peak])
    extras = extras.reshape(2, local_experts, groups, capacity).transpose(2, 0, 1, 3)
    back_narrow, back_extras = (
        lax.all_to_all(narrow, "ep", split_axis=0, concat_axis=0, tiled=True),
        lax.all_to_all(extras, "ep", split_axis=0, concat_axis=0, tiled=True),
    )
    back_product = back_extras[:, 0].reshape(slot_count)
    back_peak = back_extras[:, 1].reshape(slot_count)
    back_grad = back_narrow.reshape(slot_count, model_width).astype(jnp.float32) * back_peak[:, None]
    coarse = lax.reduce_precision(back_grad, 8, 7)
    fine = (back_grad - coarse).astype(jnp.bfloat16)
    coarse = coarse.astype(jnp.bfloat16)
    all_slots = jnp.arange(slot_count, dtype=jnp.int32)
    slot_match = token_slot[:, :, None] == all_slots[None, None, :]
    spread = jnp.any(slot_match, axis=1).astype(jnp.bfloat16)
    token_grad = jnp.dot(spread, coarse, preferred_element_type=jnp.float32) + jnp.dot(
        spread, fine, preferred_element_type=jnp.float32
    )
    pair_product = jnp.sum(jnp.where(slot_match, back_product[None, None, :], 0.0), axis=2)
    pair_product = pair_product.reshape(pair_count)
    total_grad, total_product = lax.psum((token_grad, pair_product), "tp")
    tokens_grad = total_grad.astype(jnp.bfloat16)
    gates_grad = (total_product / gate_weights.reshape(pair_count)).reshape(token_count, top_count)
    return (tokens_grad, gates_grad, gate_grad, up_grad, down_grad)


def solution(mesh):
    in_specs = (
        P("ep", None),
        P("ep", None),
        P("ep", None),
        P("ep", None),
        P("ep", None, "tp"),
        P("ep", None, "tp"),
        P("ep", "tp", None),
    )
    out_specs = (
        P("ep", None),
        P("ep", None),
        P("ep", None, "tp"),
        P("ep", None, "tp"),
        P("ep", "tp", None),
    )
    return jax.shard_map(shards, mesh=mesh, in_specs=in_specs, out_specs=out_specs, check_vma=False)
```

```python
import jax
import jax.numpy as jnp
from jax import lax
from jax.sharding import PartitionSpec as P


def expert_terms(expert_rows, expert_scaled, gate_proj, up_proj, down_proj):
    gate_pre = jnp.einsum(
        "erd,edf->erf", expert_rows, gate_proj, preferred_element_type=jnp.float32
    ).astype(jnp.bfloat16)
    up_pre = jnp.einsum(
        "erd,edf->erf", expert_rows, up_proj, preferred_element_type=jnp.float32
    ).astype(jnp.bfloat16)
    gate_pre, up_pre = lax.optimization_barrier((gate_pre, up_pre))
    hidden_grad = jnp.einsum(
        "erd,efd->erf", expert_scaled, down_proj, preferred_element_type=jnp.float32
    )
    gate_wide = gate_pre.astype(jnp.float32)
    up_wide = up_pre.astype(jnp.float32)
    sigmoid_gate = jax.nn.sigmoid(gate_wide)
    activated = gate_wide * sigmoid_gate
    hidden = activated * up_wide
    product = jnp.sum(hidden_grad * hidden, axis=-1)
    gate_pre_grad = (
        hidden_grad * up_wide * sigmoid_gate * (1.0 + gate_wide * (1.0 - sigmoid_gate))
    ).astype(jnp.bfloat16)
    up_pre_grad = (hidden_grad * activated).astype(jnp.bfloat16)
    input_grad = jnp.einsum(
        "erf,edf->erd", gate_pre_grad, gate_proj, preferred_element_type=jnp.float32
    )
    input_grad = input_grad + jnp.einsum(
        "erf,edf->erd", up_pre_grad, up_proj, preferred_element_type=jnp.float32
    )
    down_grad = jnp.einsum(
        "erf,erd->efd",
        hidden.astype(jnp.bfloat16),
        expert_scaled,
        preferred_element_type=jnp.float32,
    )
    gate_grad = jnp.einsum(
        "erd,erf->edf", expert_rows, gate_pre_grad, preferred_element_type=jnp.float32
    )
    up_grad = jnp.einsum(
        "erd,erf->edf", expert_rows, up_pre_grad, preferred_element_type=jnp.float32
    )
    return (input_grad, product, gate_grad, up_grad, down_grad)


def narrowed(values):
    peak = jnp.maximum(jnp.max(jnp.abs(values), axis=-1), 1e-30)
    return (values * (1.0 / peak)[:, :, None]).astype(jnp.float16), peak


def shards(tokens, cotangent, routing, gate_weights, gate_proj, up_proj, down_proj):
    token_count, model_width = tokens.shape
    top_count = routing.shape[1]
    local_experts = gate_proj.shape[0]
    groups = lax.axis_size("ep")
    members = lax.axis_size("tp")
    experts = local_experts * groups
    capacity = members * (
        (3 * token_count * top_count + experts * members - 1) // (experts * members)
    )
    slot_count = experts * capacity
    pair_count = token_count * top_count
    pair_expert = routing.reshape(pair_count)
    onehot = (pair_expert[:, None] == jnp.arange(experts, dtype=jnp.int32)[None, :]).astype(
        jnp.int32
    )
    position = jnp.sum(jnp.cumsum(onehot, axis=0) * onehot, axis=1) - 1
    pair_slot = pair_expert * capacity + position
    token_slot = pair_slot.reshape(token_count, top_count)
    quarter = capacity // members
    quarter_start = lax.axis_index("tp") * quarter
    slot_ids = (
        jnp.arange(experts, dtype=jnp.int32)[:, None] * capacity
        + quarter_start
        + jnp.arange(quarter, dtype=jnp.int32)[None, :]
    ).reshape(experts * quarter)
    pick = jnp.zeros((experts * quarter, token_count), jnp.bool_)
    pick_weight = jnp.zeros((experts * quarter, token_count), jnp.float32)
    for k in range(top_count):
        match = token_slot[:, k][None, :] == slot_ids[:, None]
        pick = pick | match
        pick_weight = jnp.where(match, gate_weights[:, k][None, :], pick_weight)
    pick = pick.astype(jnp.bfloat16)
    slot_weight = jnp.sum(pick_weight, axis=1)
    layout = (groups, local_experts, quarter, model_width)
    part_rows = jnp.dot(pick, tokens, preferred_element_type=jnp.float32)
    part_rows = part_rows.astype(jnp.bfloat16).reshape(layout)
    part_scaled = jnp.dot(pick, cotangent, preferred_element_type=jnp.float32)
    part_scaled = (slot_weight[:, None] * part_scaled).astype(jnp.bfloat16).reshape(layout)
    landed = (
        lax.all_to_all(part_rows, "ep", split_axis=0, concat_axis=0, tiled=True),
        lax.all_to_all(part_scaled, "ep", split_axis=0, concat_axis=0, tiled=True),
    )
    recv_rows, recv_scaled = (
        lax.all_gather(landed[0], "tp", axis=2, tiled=True),
        lax.all_gather(landed[1], "tp", axis=2, tiled=True),
    )
    expert_rows = recv_rows.transpose(1, 0, 2, 3).reshape(
        local_experts, groups * capacity, model_width
    )
    expert_scaled = recv_scaled.transpose(1, 0, 2, 3).reshape(
        local_experts, groups * capacity, model_width
    )
    input_grad, product, gate_grad, up_grad, down_grad = expert_terms(
        expert_rows, expert_scaled, gate_proj, up_proj, down_proj
    )
    half = model_width // 2
    parity = lax.axis_index("tp") % 2
    twins = [(member, member ^ 1) for member in range(members)]
    own = lax.dynamic_slice_in_dim(input_grad, parity * half, half, 2)
    other = lax.dynamic_slice_in_dim(input_grad, (1 - parity) * half, half, 2)
    other_narrow, other_peak = narrowed(other)
    twin_narrow = lax.ppermute(other_narrow, "tp", twins)
    twin_extras = lax.ppermute(jnp.stack([product, other_peak]), "tp", twins)
    own = own + twin_narrow.astype(jnp.float32) * twin_extras[1][:, :, None]
    product = product + twin_extras[0]
    narrow, peak = narrowed(own)
    narrow = narrow.reshape(local_experts, groups, capacity, half).transpose(1, 0, 2, 3)
    extras = jnp.stack([product, peak])
    extras = extras.reshape(2, local_experts, groups, capacity).transpose(2, 0, 1, 3)
    back_narrow, back_extras = (
        lax.all_to_all(narrow, "ep", split_axis=0, concat_axis=0, tiled=True),
        lax.all_to_all(extras, "ep", split_axis=0, concat_axis=0, tiled=True),
    )
    back_product = back_extras[:, 0].reshape(slot_count)
    back_peak = back_extras[:, 1].reshape(slot_count)
    back_grad = back_narrow.reshape(slot_count, half).astype(jnp.float32) * back_peak[:, None]
    coarse = lax.reduce_precision(back_grad, 8, 7)
    fine = (back_grad - coarse).astype(jnp.bfloat16)
    coarse = coarse.astype(jnp.bfloat16)
    all_slots = jnp.arange(slot_count, dtype=jnp.int32)
    slot_match = token_slot[:, :, None] == all_slots[None, None, :]
    spread = jnp.any(slot_match, axis=1).astype(jnp.bfloat16)
    token_grad = jnp.dot(spread, coarse, preferred_element_type=jnp.float32) + jnp.dot(
        spread, fine, preferred_element_type=jnp.float32
    )
    pair_product = jnp.sum(jnp.where(slot_match, back_product[None, None, :], 0.0), axis=2)
    pair_product = pair_product.reshape(pair_count)
    total_grad, total_product = token_grad, pair_product
    for step in range(2, members, 2):
        across = [(member, (member + step) % members) for member in range(members)]
        total_grad = total_grad + lax.ppermute(token_grad, "tp", across)
        total_product = total_product + lax.ppermute(pair_product, "tp", across)
    own_half = total_grad.astype(jnp.bfloat16)
    twin_half = lax.ppermute(own_half, "tp", twins)
    tokens_grad = jnp.where(
        parity == 0,
        jnp.concatenate([own_half, twin_half], axis=1),
        jnp.concatenate([twin_half, own_half], axis=1),
    )
    gates_grad = (total_product / gate_weights.reshape(pair_count)).reshape(token_count, top_count)
    return (tokens_grad, gates_grad, gate_grad, up_grad, down_grad)


def solution(mesh):
    in_specs = (
        P("ep", None),
        P("ep", None),
        P("ep", None),
        P("ep", None),
        P("ep", None, "tp"),
        P("ep", None, "tp"),
        P("ep", "tp", None),
    )
    out_specs = (
        P("ep", None),
        P("ep", None),
        P("ep", None, "tp"),
        P("ep", None, "tp"),
        P("ep", "tp", None),
    )
    return jax.shard_map(shards, mesh=mesh, in_specs=in_specs, out_specs=out_specs, check_vma=False)
```
